32 devices in a mesh: sp: 8 (over z, x), tp: 4 (over y, core).
Axes of the slice: x: 2, y: 2, z: 4, core: 2. Of those that a mesh axis runs over, the one named last changes fastest.
Arguments:
- tokens: bfloat16 [4096, 2048], P(('sp', 'tp')), may hold values from -6 to 6
- input_gain: bfloat16 [2048], replicated, may hold values from 0.099609375 to 1.8984375
- weight_query: bfloat16 [2048, 1024], P(None, 'tp'), may hold values from -0.125 to 0.125
- weight_key: bfloat16 [2048, 1024], P(None, 'tp'), may hold values from -0.125 to 0.125
- weight_value: bfloat16 [2048, 2048], P(None, 'tp'), may hold values from -8 to 8
- weight_outgate: bfloat16 [2048, 2048], P(None, 'tp'), may hold values from -0.125 to 0.125
- weight_ingate: bfloat16 [2048, 8], replicated, may hold values from -0.125 to 0.125
- weight_forget: bfloat16 [2048, 8], replicated, may hold values from -0.125 to 0.125
- forget_shift: float32 [4096, 8], P('sp', 'tp'), may hold values from 0 to 20
- mem_gain: bfloat16 [2048], replicated, may hold values from 0.099609375 to 1.8984375
- query_down_weight: bfloat16 [2048, 768], P(None, 'tp'), may hold values from -0.125 to 0.125
- latent_down_weight: bfloat16 [2048, 512], P(None, 'tp'), may hold values from -0.125 to 0.125
- down_rotary: bfloat16 [2048, 64], replicated, may hold values from -0.125 to 0.125
- query_gain: float32 [768], replicated, may hold values from 0.15 to 12
- latent_gain: float32 [512], replicated, may hold values from 0.15 to 12
- query_up_weight: bfloat16 [768, 1536], P(None, 'tp'), may hold values from -0.4375 to 0.4375
- key_up_weight: bfloat16 [512, 1024], P(None, 'tp'), may hold values from -0.25 to 0.25
- value_up_weight: bfloat16 [512, 1024], P(None, 'tp'), may hold values from -0.25 to 0.25
- out_memory: bfloat16 [2048, 2048], P('tp'), may hold values from -0.5 to 0.5
- out_attend: bfloat16 [1024, 2048], P('tp'), may hold values from -0.75 to 0.75
Outputs:
- mixed: bfloat16 [4096, 2048], P(('sp', 'tp'))
The draws below stay inside these ranges and needn't reach their ends.
All inputs are finite; a program needn't handle non-finite values.
Results may differ from the reference program's by a relative error of at most 0.04.
The reference program's roundings to bfloat16 on the way count: a program that leaves them out, or rounds other values in their place, can miss the bound.
Values may be sent and summed in bfloat16 or wider, within the bound.
A program may use at most 128 MiB of HBM per device.

```python
import jax
import jax.numpy as jnp
from jax import lax

MODEL_WIDTH = 2048
MEMORY_HEADS = 8
M_QK = 128
M_V = 256
ATTEND_HEADS = 8
PLAIN_CHANNELS = 128
ROTARY_CHANNELS = 64
VALUE_CHANNELS = 128
QUERY_LATENT = 768
LATENT_WIDTH = 512
BLOCK = 64
TOK_DEV = 512
SEQUENCE_LENGTH = 4096
N_TP = 4


def draw_forget_shift(key, part):
    random_keys = jax.random.split(key, 5)
    shuffled = jax.random.permutation(random_keys[0], MEMORY_HEADS)
    quick_heads = shuffled[:MEMORY_HEADS // 2]
    fast_head = jnp.any(jnp.arange(MEMORY_HEADS)[None, :] == quick_heads[:, None], axis=0)
    block_total = SEQUENCE_LENGTH // TOK_DEV
    factor = jnp.exp(jax.random.uniform(random_keys[1], (block_total, MEMORY_HEADS), jnp.float32, -0.7, 0.7))
    factor = jnp.repeat(factor, TOK_DEV, axis=0)
    jitter = jnp.exp(jax.random.uniform(random_keys[2], (SEQUENCE_LENGTH, MEMORY_HEADS), jnp.float32, -0.35, 0.35))
    decay_rate = jnp.where(fast_head[None, :], 1.0 / 40.0, 0.4 / SEQUENCE_LENGTH) * factor * jitter
    score_retained = -jnp.log(jnp.expm1(decay_rate))
    spike_position = jax.random.randint(random_keys[3], (4, MEMORY_HEADS), 0, SEQUENCE_LENGTH)
    spike_retained = jax.random.uniform(random_keys[4], (4, MEMORY_HEADS), jnp.float32, 0.5, 0.8)
    spike_score = jnp.log(spike_retained / (1.0 - spike_retained))
    spike_matches = jnp.arange(SEQUENCE_LENGTH)[:, None, None] == spike_position[None, :, :]
    spike_amount = jnp.min(jnp.where(spike_matches, spike_score[None], 1000000000.0), axis=1)
    score_retained = jnp.minimum(score_retained, spike_amount)
    ratio = jnp.clip(score_retained, 0.0, 13.5) / 15.0
    return 7.5 * jnp.log((1.0 + ratio) / (1.0 - ratio))


def gain_entries(key, length):
    return 1.0 + 0.18 * jnp.clip(jax.random.normal(key, (length,), jnp.float32), -4.5, 4.5)


def draw_query_gain(key, part):
    return gain_entries(jax.random.fold_in(key, 11), QUERY_LATENT)


def draw_latent_gain(key, part):
    return gain_entries(jax.random.fold_in(key, 23), LATENT_WIDTH)


def draw_weight_value(key, part):
    position = jnp.arange(MEMORY_HEADS, dtype=jnp.float32) / max(MEMORY_HEADS - 1, 1)
    top_scale = 3.0
    head_scale = jnp.repeat(jnp.power(top_scale, position), M_V)
    base = jnp.clip(jax.random.normal(jax.random.fold_in(key, 37), (MODEL_WIDTH, MEMORY_HEADS * M_V), jnp.float32), -6.0, 6.0)
    return (base * head_scale[None, :] * MODEL_WIDTH ** (-0.5)).astype(jnp.bfloat16)


def levels(key, shape, pieces, low, largest):
    level = 1.0
    for dim, parts in pieces:
        draws = jax.random.uniform(jax.random.fold_in(jax.random.fold_in(key, 6), dim), (parts,), jnp.float32, low / len(pieces), largest / len(pieces))
        level = level * jnp.repeat(jnp.exp(draws), shape[dim] // parts).reshape((-1,) + (1,) * (len(shape) - 1 - dim))
    return level


def bell_draw(key, dims, spread, most, shards=(), kind=jnp.bfloat16):
    level = levels(key, dims, shards, -0.22, 0.18) if shards else 1.0
    values = jax.random.normal(key, dims, jnp.float32) * spread * level
    return jnp.minimum(jnp.maximum(values, -most), most).astype(kind)


def setup_inputs(seed: int = 0) -> dict:
    key_list = jax.random.split(jax.random.key(seed), 21)
    tokens = bell_draw(key_list[0], (SEQUENCE_LENGTH, MODEL_WIDTH), 1.0, 6.0, ((0, 32),))
    input_gain = jnp.clip(1.0 + 0.18 * jax.random.normal(key_list[1], (MODEL_WIDTH,), jnp.float32), 0.099609375, 1.8984375).astype(jnp.bfloat16)
    weight_query = bell_draw(key_list[2], (MODEL_WIDTH, MEMORY_HEADS * M_QK), MODEL_WIDTH ** -0.5, 0.125, ((1, 4),))
    weight_key = bell_draw(key_list[3], (MODEL_WIDTH, MEMORY_HEADS * M_QK), MODEL_WIDTH ** -0.5, 0.125, ((1, 4),))
    weight_value = draw_weight_value(jax.random.fold_in(key_list[20], 71), 0)
    weight_outgate = bell_draw(key_list[5], (MODEL_WIDTH, MEMORY_HEADS * M_V), MODEL_WIDTH ** -0.5, 0.125, ((1, 4),))
    weight_ingate = bell_draw(key_list[6], (MODEL_WIDTH, MEMORY_HEADS), MODEL_WIDTH ** -0.5, 0.125)
    weight_forget = bell_draw(key_list[7], (MODEL_WIDTH, MEMORY_HEADS), MODEL_WIDTH ** -0.5, 0.125)
    forget_shift = draw_forget_shift(jax.random.fold_in(key_list[20], 71), 0)
    mem_gain = jnp.clip(1.0 + 0.18 * jax.random.normal(key_list[9], (MEMORY_HEADS * M_V,), jnp.float32), 0.099609375, 1.8984375).astype(jnp.bfloat16)
    query_down_weight = bell_draw(key_list[10], (MODEL_WIDTH, QUERY_LATENT), MODEL_WIDTH ** -0.5, 0.125, ((1, 4),))
    latent_down_weight = bell_draw(key_list[11], (MODEL_WIDTH, LATENT_WIDTH), MODEL_WIDTH ** -0.5, 0.125, ((1, 4),))
    down_rotary = bell_draw(key_list[12], (MODEL_WIDTH, ROTARY_CHANNELS), MODEL_WIDTH ** -0.5, 0.125)
    query_gain = draw_query_gain(jax.random.fold_in(key_list[20], 71), 0)
    latent_gain = draw_latent_gain(jax.random.fold_in(key_list[20], 71), 0)
    query_up_weight = bell_draw(key_list[15], (QUERY_LATENT, ATTEND_HEADS * (PLAIN_CHANNELS + ROTARY_CHANNELS)), (QUERY_LATENT // 4) ** -0.5, 0.4375, ((1, 4),))
    key_up_weight = bell_draw(key_list[16], (LATENT_WIDTH, ATTEND_HEADS * PLAIN_CHANNELS), LATENT_WIDTH ** -0.5, 0.25, ((1, 4),))
    value_up_weight = bell_draw(key_list[17], (LATENT_WIDTH, ATTEND_HEADS * VALUE_CHANNELS), LATENT_WIDTH ** -0.5, 0.25, ((1, 4),))
    out_memory = bell_draw(key_list[18], (MEMORY_HEADS * M_V, MODEL_WIDTH), (MEMORY_HEADS * M_V // 16) ** -0.5, 0.5, ((0, 4),))
    out_attend = bell_draw(key_list[19], (ATTEND_HEADS * VALUE_CHANNELS, MODEL_WIDTH), (ATTEND_HEADS * VALUE_CHANNELS // 16) ** -0.5, 0.75, ((0, 4),))
    return dict(tokens=tokens, input_gain=input_gain, weight_query=weight_query, weight_key=weight_key, weight_value=weight_value, weight_outgate=weight_outgate, weight_ingate=weight_ingate, weight_forget=weight_forget, forget_shift=forget_shift, mem_gain=mem_gain, query_down_weight=query_down_weight, latent_down_weight=latent_down_weight, down_rotary=down_rotary, query_gain=query_gain, latent_gain=latent_gain, query_up_weight=query_up_weight, key_up_weight=key_up_weight, value_up_weight=value_up_weight, out_memory=out_memory, out_attend=out_attend)


SMALL_CONSTANT = 1e-06
SOFTCAP = 15.0
ROTARY_BASE = 10000.0
PRECISE = lax.Precision.HIGHEST

def rms_scale(values, gain):
    widened = values.astype(jnp.float32)
    return widened * lax.rsqrt(lax.optimization_barrier(jnp.mean(widened * widened, axis=-1, keepdims=True)) + SMALL_CONSTANT) * gain.astype(jnp.float32)

def rotate(values, positions):
    halfway = values.shape[-1] // 2
    inverse = jnp.power(ROTARY_BASE, -jnp.arange(halfway, dtype=jnp.float32) / halfway)
    angles = positions.astype(jnp.float32)[:, None] * inverse
    cosine = jnp.cos(angles)
    sine_part = jnp.sin(angles)
    if values.ndim == 3:
        cosine = cosine[:, None, :]
        sine_part = sine_part[:, None, :]
    widened = values.astype(jnp.float32)
    first = widened[..., :halfway]
    second = widened[..., halfway:]
    turned = jnp.concatenate([first * cosine - second * sine_part, second * cosine + first * sine_part], axis=-1)
    return turned.astype(jnp.bfloat16)

def update_state(carried, key_rows, value_rows, input_gate, cumulative):
    matrix, normal, stabilizer = carried
    last_total = cumulative[:, -1]
    weight_log = last_total[:, None] - cumulative + input_gate
    new_max = jnp.maximum(last_total + stabilizer, lax.optimization_barrier(jnp.max(weight_log, axis=-1)))
    weights = jnp.exp(weight_log - new_max[:, None])
    decay = jnp.exp(last_total + stabilizer - new_max)
    matrix = decay[:, None, None] * matrix + jnp.einsum('hsv,hsd->hvd', weights[:, :, None] * value_rows, key_rows, precision=PRECISE)
    normal = decay[:, None] * normal + jnp.einsum('hs,hsd->hd', weights, key_rows, precision=PRECISE)
    return (matrix, normal, new_max)

def block_step(carried, inputs):
    query_rows, key_rows, value_rows, input_gate, log_forget = inputs
    matrix, normal, stabilizer = carried
    cumulative = jnp.cumsum(log_forget, axis=-1)
    block_len = log_forget.shape[-1]
    causal = jnp.tril(jnp.ones((block_len, block_len), dtype=bool))
    pair_log = cumulative[:, :, None] - cumulative[:, None, :] + input_gate[:, None, :]
    pair_log = jnp.where(causal, pair_log, -jnp.inf)
    carried_log = cumulative + stabilizer[:, None]
    row_max = jnp.maximum(carried_log, lax.optimization_barrier(jnp.max(pair_log, axis=-1)))
    within = jnp.exp(pair_log - row_max[:, :, None])
    across = jnp.exp(carried_log - row_max)
    affinity = jnp.einsum('hjd,hsd->hjs', query_rows, key_rows, precision=PRECISE) * within
    numerator = jnp.einsum('hjs,hsv->hjv', affinity, value_rows, precision=PRECISE)
    numerator = numerator + across[:, :, None] * jnp.einsum('hjd,hvd->hjv', query_rows, matrix, precision=PRECISE)
    denominator = lax.optimization_barrier(jnp.sum(affinity, axis=-1)) + across * jnp.einsum('hjd,hd->hj', query_rows, normal, precision=PRECISE)
    output = numerator / jnp.maximum(jnp.abs(denominator), jnp.exp(-row_max))[:, :, None]
    return (update_state(carried, key_rows, value_rows, input_gate, cumulative), output)

def memory_cell(queries, keys_in, values, input_gate, log_forget):
    length, head_count, query_width = queries.shape
    value_width = values.shape[-1]
    block_count = length // BLOCK

    def to_blocks(array, width):
        return array.astype(jnp.float32).reshape(block_count, BLOCK, head_count, width).transpose(0, 2, 1, 3)

    def gate_blocks(array):
        return array.reshape(block_count, BLOCK, head_count).transpose(0, 2, 1)
    initial = (jnp.zeros((head_count, value_width, query_width), jnp.float32), jnp.zeros((head_count, query_width), jnp.float32), jnp.zeros((head_count,), jnp.float32))
    inputs = (to_blocks(queries, query_width), to_blocks(keys_in, query_width) * query_width ** (-0.5), to_blocks(values, value_width), gate_blocks(input_gate), gate_blocks(log_forget))
    _, outputs = lax.scan(block_step, initial, inputs)
    return outputs.transpose(0, 2, 1, 3).reshape(length, head_count, value_width)

def latent_attention(queries, key_nope, key_rot, values):
    length = queries.shape[0]
    size = min(512, length)
    factor = (PLAIN_CHANNELS + ROTARY_CHANNELS) ** (-0.5)
    results = []
    for block_number in range(length // size):
        lower = block_number * size
        upper = lower + size
        query_nope = queries[lower:upper, :, :PLAIN_CHANNELS].astype(jnp.float32)
        query_rot = queries[lower:upper, :, PLAIN_CHANNELS:].astype(jnp.float32)
        scores = jnp.einsum('qhd,khd->hqk', query_nope, key_nope[:upper].astype(jnp.float32))
        scores = (scores + jnp.einsum('qhd,kd->hqk', query_rot, key_rot[:upper].astype(jnp.float32))) * factor
        allowed = jnp.arange(upper)[None, :] <= (lower + jnp.arange(size))[:, None]
        scores = jnp.where(allowed[None], scores, -jnp.inf)
        row_max = lax.optimization_barrier(jnp.max(scores, axis=-1, keepdims=True))
        probs = jnp.exp(scores - row_max)
        summed = lax.optimization_barrier(jnp.sum(probs, axis=-1))
        rounded = lax.optimization_barrier(probs.astype(jnp.bfloat16)).astype(jnp.float32)
        numerator = jnp.einsum('hqk,khd->qhd', rounded, values[:upper].astype(jnp.float32))
        results.append((numerator / summed.T[:, :, None]).astype(jnp.bfloat16))
    return jnp.concatenate(results, axis=0)

def reference(tokens, input_gain, weight_query, weight_key, weight_value, weight_outgate, weight_ingate, weight_forget, forget_shift, mem_gain, query_down_weight, latent_down_weight, down_rotary, query_gain, latent_gain, query_up_weight, key_up_weight, value_up_weight, out_memory, out_attend):
    length = tokens.shape[0]
    normed = rms_scale(tokens, input_gain).astype(jnp.bfloat16)

    def project(weight):
        return jnp.dot(normed, weight, preferred_element_type=jnp.float32)
    stored = (project(weight_query).astype(jnp.bfloat16), project(weight_key).astype(jnp.bfloat16), project(weight_value).astype(jnp.bfloat16), project(weight_outgate).astype(jnp.bfloat16))
    mem_query, mem_key, mem_value, mem_outgate = lax.optimization_barrier(stored)
    in_pre = project(weight_ingate)
    forget_pre = project(weight_forget) + forget_shift
    in_gate = SOFTCAP * jnp.tanh(in_pre / SOFTCAP)
    log_forget = jax.nn.log_sigmoid(SOFTCAP * jnp.tanh(forget_pre / SOFTCAP))
    query_latent = project(query_down_weight).astype(jnp.bfloat16)
    keyval_latent = project(latent_down_weight).astype(jnp.bfloat16)
    key_raw = project(down_rotary).astype(jnp.bfloat16)
    positions = jnp.arange(length, dtype=jnp.int32)
    cell = memory_cell(mem_query.reshape(length, MEMORY_HEADS, M_QK), mem_key.reshape(length, MEMORY_HEADS, M_QK), mem_value.reshape(length, MEMORY_HEADS, M_V), in_gate, log_forget)
    cell = cell.reshape(length, MEMORY_HEADS * M_V)
    gated = rms_scale(cell, mem_gain)
    gated = gated * jax.nn.sigmoid(mem_outgate.astype(jnp.float32))
    gated = gated.astype(jnp.bfloat16)
    normed_query = rms_scale(query_latent, query_gain).astype(jnp.bfloat16)
    normed_latent = rms_scale(keyval_latent, latent_gain).astype(jnp.bfloat16)
    query_all = jnp.dot(normed_query, query_up_weight, preferred_element_type=jnp.float32).astype(jnp.bfloat16)
    query_all = query_all.reshape(length, ATTEND_HEADS, PLAIN_CHANNELS + ROTARY_CHANNELS)
    queries = jnp.concatenate([query_all[..., :PLAIN_CHANNELS], rotate(query_all[..., PLAIN_CHANNELS:], positions)], axis=-1)
    key_nope = jnp.dot(normed_latent, key_up_weight, preferred_element_type=jnp.float32).astype(jnp.bfloat16)
    values = jnp.dot(normed_latent, value_up_weight, preferred_element_type=jnp.float32).astype(jnp.bfloat16)
    key_rot = rotate(key_raw, positions)
    attended = latent_attention(queries, key_nope.reshape(length, ATTEND_HEADS, PLAIN_CHANNELS), key_rot, values.reshape(length, ATTEND_HEADS, VALUE_CHANNELS)).reshape(length, ATTEND_HEADS * VALUE_CHANNELS)
    mem_share = MEMORY_HEADS // N_TP * M_V
    att_share = ATTEND_HEADS // N_TP * VALUE_CHANNELS
    summed = jnp.zeros((length, tokens.shape[1]), jnp.float32)
    for share in range(N_TP):
        partial_value = jnp.dot(gated[:, share * mem_share:(share + 1) * mem_share], out_memory[share * mem_share:(share + 1) * mem_share], preferred_element_type=jnp.float32)
        partial_value = partial_value + jnp.dot(attended[:, share * att_share:(share + 1) * att_share], out_attend[share * att_share:(share + 1) * att_share], preferred_element_type=jnp.float32)
        summed = summed + lax.optimization_barrier(partial_value.astype(jnp.bfloat16)).astype(jnp.float32)
    return summed.astype(jnp.bfloat16)
```

```python
import functools
import math

import jax
import jax.numpy as jnp
from jax import lax
from jax.experimental import pallas as pl
from jax.experimental.pallas import tpu as pltpu
from jax.sharding import PartitionSpec as P

MEMORY_HEADS = 8
M_QK = 128
M_V = 256
PLAIN_CHANNELS = 128
ROTARY_CHANNELS = 64
VALUE_CHANNELS = 128
HEAD_WIDTH = PLAIN_CHANNELS + ROTARY_CHANNELS
SMALL_CONSTANT = 1e-06
SOFTCAP = 15.0
ROTARY_BASE = 10000.0
FAR_BELOW = -1e30
EXTRA_ROWS = 16
F32 = jnp.float32
BF16 = jnp.bfloat16
VMEM_LIMIT = 56 * 1024 * 1024
NT = (((1,), (1,)), ((), ()))
TN = (((0,), (0,)), ((), ()))


def dot(a, b):
    return jnp.dot(a, b, preferred_element_type=F32)


def rms_scale(values, gain):
    widened = values.astype(F32)
    return (
        widened
        * lax.rsqrt(jnp.mean(widened * widened, axis=-1, keepdims=True) + SMALL_CONSTANT)
        * gain.astype(F32)
    )


def split3(value):
    high = value.astype(BF16)
    rest = value - high.astype(F32)
    middle = rest.astype(BF16)
    low = (rest - middle.astype(F32)).astype(BF16)
    return high, middle, low


def local_memory(heads, query_ref, key_ref, value_ref, small_ref, shift_ref,
                 num_ref, stats_ref, state_ref, extra_ref):
    length = query_ref.shape[0]
    scale = M_QK ** -0.5
    gate = small_ref[:, ROTARY_CHANNELS:ROTARY_CHANNELS + heads]
    forget = small_ref[:, ROTARY_CHANNELS + heads:ROTARY_CHANNELS + 2 * heads] + shift_ref[...]
    gate = SOFTCAP * jnp.tanh(gate / SOFTCAP)
    capped = SOFTCAP * jnp.tanh(forget / SOFTCAP)
    log_forget = jnp.minimum(capped, 0.0) - jnp.log1p(jnp.exp(-jnp.abs(capped)))
    row = lax.broadcasted_iota(jnp.int32, (length, length), 0)
    col = lax.broadcasted_iota(jnp.int32, (length, length), 1)
    causal = col <= row
    cumulative = jnp.dot(
        causal.astype(F32), log_forget, preferred_element_type=F32,
        precision=lax.Precision.HIGHEST,
    )
    offset = gate - cumulative
    lanes = jnp.concatenate(
        [offset, jnp.zeros((length, 128 - heads), F32)], axis=1
    )
    offset_rows = lanes.T
    stats = []
    extras = []
    for h in range(heads):
        q = query_ref[:, h * M_QK:(h + 1) * M_QK]
        k = key_ref[:, h * M_QK:(h + 1) * M_QK]
        v = value_ref[:, h * M_V:(h + 1) * M_V]
        b = cumulative[:, h:h + 1]
        w = offset_rows[h:h + 1, :]
        masked = jnp.where(causal, w, -jnp.inf)
        top = jnp.max(masked, axis=1, keepdims=True)
        weight = jnp.exp(masked - top)
        affinity = lax.dot_general(q, k, NT, preferred_element_type=F32) * (weight * scale)
        num_ref[:, h * M_V:(h + 1) * M_V] = dot(affinity.astype(BF16), v)
        stats += [b, b + top, jnp.sum(affinity, axis=1, keepdims=True)]
        last = b[length - 1:length, :]
        best = top[length - 1:length, :]
        decay = jnp.exp(offset[:, h:h + 1] - best) * scale
        state_ref[h * M_V:(h + 1) * M_V, :] = lax.dot_general(
            (decay * v.astype(F32)).astype(BF16), k, TN, preferred_element_type=F32
        ).astype(BF16)
        normal = jnp.sum(decay * k.astype(F32), axis=0, keepdims=True)
        parts = split3(normal) + split3(jnp.broadcast_to(last + best, (1, 128))) + split3(
            jnp.broadcast_to(last, (1, 128))
        )
        extras += [part.astype(F32) for part in parts]
    stats_ref[...] = jnp.concatenate(
        stats + [jnp.zeros((length, 128 - 3 * heads), F32)], axis=1
    )
    count = len(extras)
    rows = extra_ref.shape[0]
    extra_ref[...] = jnp.concatenate(
        extras + [jnp.zeros((rows - count, 128), F32)], axis=0
    ).astype(BF16)


def rotated(values, cosine, sine):
    half = values.shape[-1] // 2
    widened = values.astype(F32)
    first = widened[:, :half]
    second = widened[:, half:]
    return jnp.concatenate(
        [first * cosine - second * sine, second * cosine + first * sine], axis=1
    ).astype(BF16)


def prepare(heads, latents_ref, small_ref, cos_ref, sin_ref, qgain_ref, lgain_ref,
            qup_ref, kup_ref, vup_ref, state_ref, extra_ref, query_ref, pack_ref):
    shares, length, _ = latents_ref.shape
    lat_part = lgain_ref.shape[1]
    q_part = qgain_ref.shape[1]
    lat_sum = 0.0
    q_sum = 0.0
    for t in range(shares):
        a = latents_ref[t, :, :lat_part].astype(F32)
        b = latents_ref[t, :, lat_part:].astype(F32)
        lat_sum = lat_sum + jnp.sum(a * a, axis=1, keepdims=True)
        q_sum = q_sum + jnp.sum(b * b, axis=1, keepdims=True)
    lat_rs = lax.rsqrt(lat_sum / (shares * lat_part) + SMALL_CONSTANT)
    q_rs = lax.rsqrt(q_sum / (shares * q_part) + SMALL_CONSTANT)
    query = 0.0
    keys = 0.0
    values = 0.0
    for t in range(shares):
        a = latents_ref[t, :, :lat_part].astype(F32)
        b = latents_ref[t, :, lat_part:].astype(F32)
        a = (a * lat_rs * lgain_ref[t:t + 1, :]).astype(BF16)
        b = (b * q_rs * qgain_ref[t:t + 1, :]).astype(BF16)
        query = query + dot(b, qup_ref[t * q_part:(t + 1) * q_part, :])
        keys = keys + dot(a, kup_ref[t * lat_part:(t + 1) * lat_part, :])
        values = values + dot(a, vup_ref[t * lat_part:(t + 1) * lat_part, :])
    query = query.astype(BF16)
    cosine = cos_ref[...]
    sine = sin_ref[...]
    for h in range(heads):
        base = h * HEAD_WIDTH
        query_ref[h, :, :PLAIN_CHANNELS] = query[:, base:base + PLAIN_CHANNELS]
        query_ref[h, :, PLAIN_CHANNELS:] = rotated(
            query[:, base + PLAIN_CHANNELS:base + HEAD_WIDTH], cosine, sine
        )
    width_k = keys.shape[1]
    width_v = values.shape[1]
    pack_ref[:length, :width_k] = keys.astype(BF16)
    pack_ref[:length, width_k:width_k + width_v] = values.astype(BF16)
    base = width_k + width_v
    filled = state_ref.shape[0]
    pack_ref[:filled, base:base + 128] = state_ref[...]
    if filled < length:
        pack_ref[filled:length, base:base + 128] = jnp.zeros((length - filled, 128), BF16)
    pack_ref[:length, base + 128:] = rotated(
        small_ref[:, :ROTARY_CHANNELS].astype(BF16), cosine, sine
    )
    rows = extra_ref.shape[0]
    pack_ref[length:, :] = jnp.zeros((rows, pack_ref.shape[1]), BF16)
    pack_ref[length:, :128] = extra_ref[...]


def mixers(mem_heads, att_heads, where_ref, pack_ref, query_ref, memq_ref, num_ref, stats_ref,
           cell_ref, square_ref, attended_ref,
           top_ref, sum_ref, acc_ref, matrix_ref, normal_ref, stab_ref):
    step = pl.program_id(0)
    mine = where_ref[0]
    length = query_ref.shape[1]
    factor = HEAD_WIDTH ** -0.5
    width_k = att_heads * PLAIN_CHANNELS
    width_v = att_heads * VALUE_CHANNELS
    base = width_k + width_v

    @pl.when(step == 0)
    def _():
        top_ref[...] = jnp.full(top_ref.shape, FAR_BELOW, F32)
        sum_ref[...] = jnp.zeros(sum_ref.shape, F32)
        acc_ref[...] = jnp.zeros(acc_ref.shape, F32)
        matrix_ref[...] = jnp.zeros(matrix_ref.shape, F32)
        normal_ref[...] = jnp.zeros(normal_ref.shape, F32)
        stab_ref[...] = jnp.zeros(stab_ref.shape, F32)

    def attend(masked):
        rotary = pack_ref[0, :length, base + 128:]
        for h in range(att_heads):
            key = jnp.concatenate(
                [pack_ref[0, :length, h * PLAIN_CHANNELS:(h + 1) * PLAIN_CHANNELS], rotary], axis=1
            )
            scores = lax.dot_general(query_ref[h], key, NT, preferred_element_type=F32)
            if masked:
                row = lax.broadcasted_iota(jnp.int32, scores.shape, 0)
                col = lax.broadcasted_iota(jnp.int32, scores.shape, 1)
                scores = jnp.where(col <= row, scores, FAR_BELOW)
            old = top_ref[h, :, :1]
            new = jnp.maximum(old, jnp.max(scores, axis=1, keepdims=True))
            probs = jnp.exp((scores - new) * factor)
            shrink = jnp.exp((old - new) * factor)
            sum_ref[h] = sum_ref[h] * shrink + jnp.sum(probs, axis=1, keepdims=True)
            value = pack_ref[0, :length, width_k + h * VALUE_CHANNELS:width_k + (h + 1) * VALUE_CHANNELS]
            acc_ref[h] = acc_ref[h] * shrink + dot(probs.astype(BF16), value)
            top_ref[h] = jnp.broadcast_to(new, top_ref.shape[1:])

    @pl.when(step < mine)
    def _():
        attend(False)
        extra = pack_ref[0, length:, :128].astype(F32)
        state = pack_ref[0, :length, base:base + 128].astype(F32)
        pieces = [extra[9 * h + 3 * g:9 * h + 3 * g + 1] + extra[9 * h + 3 * g + 1:9 * h + 3 * g + 2]
                  + extra[9 * h + 3 * g + 2:9 * h + 3 * g + 3]
                  for h in range(mem_heads) for g in range(3)]
        for h in range(mem_heads):
            normal, best, last = pieces[3 * h:3 * h + 3]
            decayed = stab_ref[h:h + 1, :] + last
            new = jnp.maximum(decayed, best)
            early = jnp.exp(decayed - new)
            late = jnp.exp(best - new)
            rows = slice(h * M_V, (h + 1) * M_V)
            matrix_ref[rows, :] = matrix_ref[rows, :] * early + late * state[rows, :]
            normal_ref[h:h + 1, :] = normal_ref[h:h + 1, :] * early + late * normal
            stab_ref[h:h + 1, :] = new

    @pl.when(step == mine)
    def _():
        attend(True)
        for h in range(att_heads):
            attended_ref[:, h * VALUE_CHANNELS:(h + 1) * VALUE_CHANNELS] = (
                acc_ref[h] / sum_ref[h]
            ).astype(BF16)
        squares = 0.0
        for h in range(mem_heads):
            b = stats_ref[:, 3 * h:3 * h + 1]
            local = stats_ref[:, 3 * h + 1:3 * h + 2]
            local_den = stats_ref[:, 3 * h + 2:3 * h + 3]
            q = memq_ref[:, h * M_QK:(h + 1) * M_QK]
            carried = b + stab_ref[h:h + 1, :1]
            row_max = jnp.maximum(carried, local)
            across = jnp.exp(carried - row_max)
            within = jnp.exp(local - row_max)
            inter = lax.dot_general(
                q, matrix_ref[h * M_V:(h + 1) * M_V, :].astype(BF16), NT,
                preferred_element_type=F32,
            )
            dots = jnp.sum(q.astype(F32) * normal_ref[h:h + 1, :], axis=1, keepdims=True)
            den = within * local_den + across * dots
            den = jnp.maximum(jnp.abs(den), jnp.exp(-row_max))
            cell = (within * num_ref[:, h * M_V:(h + 1) * M_V] + across * inter) / den
            cell_ref[:, h * M_V:(h + 1) * M_V] = cell
            squares = squares + jnp.sum(cell * cell, axis=1, keepdims=True)
        square_ref[...] = squares


def params(**more):
    return pltpu.CompilerParams(vmem_limit_bytes=VMEM_LIMIT, **more)


def per_device(
    tokens, input_gain, weight_query, weight_key, weight_value, weight_outgate, weight_ingate,
    weight_forget, forget_shift, mem_gain, query_down_weight, latent_down_weight, down_rotary,
    query_gain, latent_gain, query_up_weight, key_up_weight, value_up_weight, out_memory,
    out_attend,
):
    tp_index = lax.axis_index("tp")
    tp = lax.axis_size("tp")
    sp = lax.axis_size("sp")
    mem_heads = weight_query.shape[1] // M_QK
    att_heads = key_up_weight.shape[1] // PLAIN_CHANNELS
    length = tokens.shape[0] * tp
    model = tokens.shape[1]
    ingate_cols = lax.dynamic_slice_in_dim(weight_ingate, tp_index * mem_heads, mem_heads, 1)
    forget_cols = lax.dynamic_slice_in_dim(weight_forget, tp_index * mem_heads, mem_heads, 1)
    small_weight = jnp.concatenate(
        [down_rotary, ingate_cols, forget_cols,
         jnp.zeros((model, 128 - ROTARY_CHANNELS - 2 * mem_heads), BF16)], axis=1
    )
    latent_weight = jnp.concatenate([latent_down_weight, query_down_weight], axis=1)
    positions = lax.axis_index("sp") * length + jnp.arange(length, dtype=jnp.int32)
    half = ROTARY_CHANNELS // 2
    inverse = jnp.power(ROTARY_BASE, -jnp.arange(half, dtype=F32) / half)
    angles = positions.astype(F32)[:, None] * inverse
    cosine = jnp.cos(angles)
    sine = jnp.sin(angles)

    normed = rms_scale(tokens, input_gain).astype(BF16)
    rows = lax.all_gather(normed, "tp", axis=0, tiled=True)
    latents = dot(rows, latent_weight).astype(BF16)
    latents_all = lax.all_gather(latents, "tp", axis=0)
    small = dot(rows, small_weight)
    mem_query = dot(rows, weight_query).astype(BF16)
    mem_key = dot(rows, weight_key).astype(BF16)
    mem_value = dot(rows, weight_value).astype(BF16)
    mem_outgate = dot(rows, weight_outgate).astype(BF16)

    extra_rows = -(-9 * mem_heads // 32) * 32
    num, stats, state, extra = pl.pallas_call(
        functools.partial(local_memory, mem_heads),
        out_shape=(
            jax.ShapeDtypeStruct((length, mem_heads * M_V), F32),
            jax.ShapeDtypeStruct((length, 128), F32),
            jax.ShapeDtypeStruct((mem_heads * M_V, 128), BF16),
            jax.ShapeDtypeStruct((extra_rows, 128), BF16),
        ),
        compiler_params=params(),
        name="local_memory",
    )(mem_query, mem_key, mem_value, small, forget_shift)

    width = att_heads * (PLAIN_CHANNELS + VALUE_CHANNELS) + 128 + ROTARY_CHANNELS
    query, pack = pl.pallas_call(
        functools.partial(prepare, att_heads),
        out_shape=(
            jax.ShapeDtypeStruct((att_heads, length, HEAD_WIDTH), BF16),
            jax.ShapeDtypeStruct((length + extra_rows, width), BF16),
        ),
        compiler_params=params(),
        name="prepare",
    )(
        latents_all, small, cosine, sine, query_gain.reshape(tp, -1), latent_gain.reshape(tp, -1),
        query_up_weight, key_up_weight, value_up_weight, state, extra,
    )
    packs = lax.all_gather(pack, "sp", axis=0)

    full = lambda shape: pl.BlockSpec(shape, lambda i, w: (0,) * len(shape))
    cell, squares, attended = pl.pallas_call(
        functools.partial(mixers, mem_heads, att_heads),
        grid_spec=pltpu.PrefetchScalarGridSpec(
            num_scalar_prefetch=1,
            grid=(sp,),
            in_specs=[
                pl.BlockSpec((1, length + extra_rows, width),
                             lambda i, w: (jnp.minimum(i, w[0]), 0, 0)),
                full(query.shape), full(mem_query.shape), full(num.shape), full(stats.shape),
            ],
            out_specs=[full((length, mem_heads * M_V)), full((length, 1)),
                       full((length, att_heads * VALUE_CHANNELS))],
            scratch_shapes=[
                pltpu.VMEM((att_heads, length, 128), F32),
                pltpu.VMEM((att_heads, length, 128), F32),
                pltpu.VMEM((att_heads, length, VALUE_CHANNELS), F32),
                pltpu.VMEM((mem_heads * M_V, 128), F32),
                pltpu.VMEM((8, 128), F32),
                pltpu.VMEM((8, 128), F32),
            ],
        ),
        out_shape=(
            jax.ShapeDtypeStruct((length, mem_heads * M_V), F32),
            jax.ShapeDtypeStruct((length, 1), F32),
            jax.ShapeDtypeStruct((length, att_heads * VALUE_CHANNELS), BF16),
        ),
        compiler_params=params(dimension_semantics=("arbitrary",)),
        name="mixers",
    )(lax.axis_index("sp").astype(jnp.int32).reshape(1), packs, query, mem_query, num, stats)

    total = lax.psum(squares, "tp")
    gain_part = lax.dynamic_slice_in_dim(mem_gain, tp_index * mem_heads * M_V, mem_heads * M_V, 0)
    gated = (
        cell * lax.rsqrt(total / (tp * mem_heads * M_V) + SMALL_CONSTANT) * gain_part.astype(F32)
        * jax.nn.sigmoid(mem_outgate.astype(F32))
    ).astype(BF16)
    partial = (dot(gated, out_memory) + dot(attended, out_attend)).astype(BF16)
    return lax.psum_scatter(partial, "tp", scatter_dimension=0, tiled=True)


def solution(mesh):
    placed = (
        P(("sp", "tp"), None), P(), P(None, "tp"), P(None, "tp"), P(None, "tp"), P(None, "tp"),
        P(), P(), P("sp", "tp"), P(), P(None, "tp"), P(None, "tp"), P(), P(), P(),
        P(None, "tp"), P(None, "tp"), P(None, "tp"), P("tp", None), P("tp", None),
    )
    return jax.shard_map(
        per_device, mesh=mesh, in_specs=placed, out_specs=P(("sp", "tp"), None), check_vma=False
    )
```

```python
import functools
import math

import jax
import jax.numpy as jnp
from jax import lax
from jax.experimental import pallas as pl
from jax.experimental.pallas import tpu as pltpu
from jax.sharding import PartitionSpec as P

MEMORY_HEADS = 8
M_QK = 128
M_V = 256
PLAIN_CHANNELS = 128
ROTARY_CHANNELS = 64
VALUE_CHANNELS = 128
HEAD_WIDTH = PLAIN_CHANNELS + ROTARY_CHANNELS
SMALL_CONSTANT = 1e-06
SOFTCAP = 15.0
ROTARY_BASE = 10000.0
FAR_BELOW = -1e30
EXTRA_ROWS = 16
F32 = jnp.float32
BF16 = jnp.bfloat16
VMEM_LIMIT = 56 * 1024 * 1024
NT = (((1,), (1,)), ((), ()))
TN = (((0,), (0,)), ((), ()))


def dot(a, b):
    return jnp.dot(a, b, preferred_element_type=F32)


def rms_scale(values, gain):
    widened = values.astype(F32)
    return (
        widened
        * lax.rsqrt(jnp.mean(widened * widened, axis=-1, keepdims=True) + SMALL_CONSTANT)
        * gain.astype(F32)
    )


def split3(value):
    high = value.astype(BF16)
    rest = value - high.astype(F32)
    middle = rest.astype(BF16)
    low = (rest - middle.astype(F32)).astype(BF16)
    return high, middle, low


def local_memory(heads, query_ref, key_ref, value_ref, small_ref, shift_ref,
                 num_ref, stats_ref, state_ref):
    length = query_ref.shape[0]
    scale = M_QK ** -0.5
    gate = small_ref[:, ROTARY_CHANNELS:ROTARY_CHANNELS + heads]
    forget = small_ref[:, ROTARY_CHANNELS + heads:ROTARY_CHANNELS + 2 * heads] + shift_ref[...]
    gate = SOFTCAP * jnp.tanh(gate / SOFTCAP)
    capped = SOFTCAP * jnp.tanh(forget / SOFTCAP)
    log_forget = jnp.minimum(capped, 0.0) - jnp.log1p(jnp.exp(-jnp.abs(capped)))
    row = lax.broadcasted_iota(jnp.int32, (length, length), 0)
    col = lax.broadcasted_iota(jnp.int32, (length, length), 1)
    causal = col <= row
    cumulative = jnp.dot(
        causal.astype(F32), log_forget, preferred_element_type=F32,
        precision=lax.Precision.HIGHEST,
    )
    offset = gate - cumulative
    lanes = jnp.concatenate(
        [offset, jnp.zeros((length, 128 - heads), F32)], axis=1
    )
    offset_rows = lanes.T
    stats = []
    extras = []
    for h in range(heads):
        q = query_ref[:, h * M_QK:(h + 1) * M_QK]
        k = key_ref[:, h * M_QK:(h + 1) * M_QK]
        v = value_ref[:, h * M_V:(h + 1) * M_V]
        b = cumulative[:, h:h + 1]
        w = offset_rows[h:h + 1, :]
        masked = jnp.where(causal, w, -jnp.inf)
        top = jnp.max(masked, axis=1, keepdims=True)
        weight = jnp.exp(masked - top)
        affinity = lax.dot_general(q, k, NT, preferred_element_type=F32) * (weight * scale)
        num_ref[:, h * M_V:(h + 1) * M_V] = dot(affinity.astype(BF16), v)
        stats += [b, b + top, jnp.sum(affinity, axis=1, keepdims=True)]
        last = b[length - 1:length, :]
        best = top[length - 1:length, :]
        decay = jnp.exp(offset[:, h:h + 1] - best) * scale
        state_ref[h * M_V:(h + 1) * M_V, :] = lax.dot_general(
            (decay * v.astype(F32)).astype(BF16), k, TN, preferred_element_type=F32
        ).astype(BF16)
        normal = jnp.sum(decay * k.astype(F32), axis=0, keepdims=True)
        parts = split3(normal) + split3(jnp.broadcast_to(last + best, (1, 128))) + split3(
            jnp.broadcast_to(last, (1, 128))
        )
        extras += [part.astype(F32) for part in parts]
    stats_ref[...] = jnp.concatenate(
        stats + [jnp.zeros((length, 128 - 3 * heads), F32)], axis=1
    )
    count = len(extras)
    rows = state_ref.shape[0] - heads * M_V
    state_ref[heads * M_V:, :] = jnp.concatenate(
        extras + [jnp.zeros((rows - count, 128), F32)], axis=0
    ).astype(BF16)


def rotated(values, cosine, sine):
    half = values.shape[-1] // 2
    widened = values.astype(F32)
    first = widened[:, :half]
    second = widened[:, half:]
    return jnp.concatenate(
        [first * cosine - second * sine, second * cosine + first * sine], axis=1
    ).astype(BF16)


def prepare(heads, latents_ref, small_ref, cos_ref, sin_ref, qgain_ref, lgain_ref,
            qup_ref, query_ref, latn_ref):
    shares, length, _ = latents_ref.shape
    lat_part = lgain_ref.shape[1]
    q_part = qgain_ref.shape[1]
    lat_sum = 0.0
    q_sum = 0.0
    for t in range(shares):
        a = latents_ref[t, :, :lat_part].astype(F32)
        b = latents_ref[t, :, lat_part:].astype(F32)
        lat_sum = lat_sum + jnp.sum(a * a, axis=1, keepdims=True)
        q_sum = q_sum + jnp.sum(b * b, axis=1, keepdims=True)
    lat_rs = lax.rsqrt(lat_sum / (shares * lat_part) + SMALL_CONSTANT)
    q_rs = lax.rsqrt(q_sum / (shares * q_part) + SMALL_CONSTANT)
    query = 0.0
    for t in range(shares):
        a = latents_ref[t, :, :lat_part].astype(F32)
        b = latents_ref[t, :, lat_part:].astype(F32)
        latn_ref[:, t * lat_part:(t + 1) * lat_part] = (a * lat_rs * lgain_ref[t:t + 1, :]).astype(BF16)
        b = (b * q_rs * qgain_ref[t:t + 1, :]).astype(BF16)
        query = query + dot(b, qup_ref[t * q_part:(t + 1) * q_part, :])
    query = query.astype(BF16)
    cosine = cos_ref[...]
    sine = sin_ref[...]
    for h in range(heads):
        base = h * HEAD_WIDTH
        query_ref[h, :, :PLAIN_CHANNELS] = query[:, base:base + PLAIN_CHANNELS]
        query_ref[h, :, PLAIN_CHANNELS:] = rotated(
            query[:, base + PLAIN_CHANNELS:base + HEAD_WIDTH], cosine, sine
        )
    latn_ref[:, shares * lat_part:] = rotated(
        small_ref[:, :ROTARY_CHANNELS].astype(BF16), cosine, sine
    )


def mixers(mem_heads, att_heads, nz, nx, tp,
           latn_ref, state_ref, query_ref, kup_ref, vup_ref, memq_ref, num_ref, stats_ref,
           cell_ref, square_ref, attended_ref,
           lat_ref, states_ref, top_ref, sum_ref, acc_ref, matrix_ref, normal_ref, stab_ref,
           recv_l, recv_s, send_lz, send_sz, send_lx, send_sx, send_ly, send_lc):
    mine = lax.axis_index("sp")
    t = lax.axis_index("tp")
    z = mine // nx
    x = lax.rem(mine, nx)
    ny = tp // 2
    y = t // 2
    core = lax.rem(t, 2)
    sibling = y * 2 + 1 - core
    length = query_ref.shape[1]
    rows = length // tp
    rank = latn_ref.shape[1] - ROTARY_CHANNELS
    factor = HEAD_WIDTH ** -0.5

    barrier = pltpu.get_barrier_semaphore()
    friends = [(mine, sibling)]
    if nz > 1:
        friends += [(lax.rem(z + 1, nz) * nx + x, t), (lax.rem(z + nz - 1, nz) * nx + x, t)]
    friends += [(z * nx + lax.rem(x + j, nx), t) for j in range(1, nx)]
    friends += [(mine, lax.rem(y + j, ny) * 2 + core) for j in range(1, ny)]
    for friend in friends:
        pl.semaphore_signal(barrier, inc=1, device_id=friend, device_id_type=pl.DeviceIdType.MESH)
    pl.semaphore_wait(barrier, len(friends))

    def remote(src, dst, send, recv, target):
        return pltpu.make_async_remote_copy(
            src_ref=src, dst_ref=dst, send_sem=send, recv_sem=recv, device_id=target,
            device_id_type=pl.DeviceIdType.MESH,
        )

    up = lax.rem(z + 1, nz) * nx + x
    own = latn_ref.at[pl.ds(pl.multiple_of(t * rows, rows), rows)]

    def quarter(slot, own_block):
        return own if own_block else lat_ref.at[slot, t]

    def state_of(slot, own_block):
        return state_ref if own_block else states_ref.at[slot]

    def to_up(slot, own_block=False):
        return [
            remote(state_of(slot, own_block), states_ref.at[slot], send_sz.at[slot],
                   recv_s.at[slot], (up, t)),
            remote(quarter(slot, own_block), lat_ref.at[slot, t], send_lz.at[slot],
                   recv_l.at[slot, t], (up, t)),
        ]

    def to_side(slot, j, own_block=False):
        target = (z * nx + lax.rem(x + j, nx), t)
        return [
            remote(state_of(slot, own_block), states_ref.at[slot], send_sx.at[slot, j],
                   recv_s.at[slot], target),
            remote(quarter(slot, own_block), lat_ref.at[slot, t], send_lx.at[slot, j],
                   recv_l.at[slot, t], target),
        ]

    def to_peer(slot, j):
        return remote(lat_ref.at[slot, t], lat_ref.at[slot, t], send_ly.at[slot, j],
                      recv_l.at[slot, t], (mine, lax.rem(y + j, ny) * 2 + core))

    def to_sibling(slot, part):
        return remote(lat_ref.at[slot, part], lat_ref.at[slot, part], send_lc.at[slot, part],
                      recv_l.at[slot, part], (mine, sibling))

    def landed(slot, part):
        remote(lat_ref.at[slot, part], lat_ref.at[slot, part], send_lc.at[slot, part],
               recv_l.at[slot, part], (mine, sibling)).wait_recv()

    def start(copies):
        for copy in copies:
            copy.start()

    def sent(copies):
        for copy in copies:
            copy.wait_send()

    def each_own(action):
        @pl.when(z < nz - 1)
        def _():
            action(to_up(mine, True))
        for j in range(1, nx):
            @pl.when(x + j < nx)
            def _():
                action(to_side(mine, j, True))

    def each_column(slot, action):
        for j in range(1, nx):
            action(to_side(slot, j))
        @pl.when(z < nz - 1)
        def _():
            action(to_up(slot))

    def each_handled(slot, action):
        action([to_peer(slot, j) for j in range(1, ny)] + [to_sibling(slot, t)])

    def arrive(slot):
        remote(states_ref.at[slot], states_ref.at[slot], send_sz.at[slot], recv_s.at[slot],
               (mine, sibling)).wait_recv()
        landed(slot, t)

    each_own(start)

    top_ref[...] = jnp.full(top_ref.shape, FAR_BELOW, F32)
    sum_ref[...] = jnp.zeros(sum_ref.shape, F32)
    acc_ref[...] = jnp.zeros(acc_ref.shape, F32)
    matrix_ref[...] = jnp.zeros(matrix_ref.shape, F32)
    normal_ref[...] = jnp.zeros(normal_ref.shape, F32)
    stab_ref[...] = jnp.zeros(stab_ref.shape, F32)

    def attend(block, masked):
        latent = block[:, :rank]
        rotary = block[:, rank:]
        keys = dot(latent, kup_ref[...]).astype(BF16)
        values = dot(latent, vup_ref[...]).astype(BF16)
        for h in range(att_heads):
            key = jnp.concatenate(
                [keys[:, h * PLAIN_CHANNELS:(h + 1) * PLAIN_CHANNELS], rotary], axis=1
            )
            scores = lax.dot_general(query_ref[h], key, NT, preferred_element_type=F32)
            if masked:
                row = lax.broadcasted_iota(jnp.int32, scores.shape, 0)
                col = lax.broadcasted_iota(jnp.int32, scores.shape, 1)
                scores = jnp.where(col <= row, scores, FAR_BELOW)
            old = top_ref[h, :, :1]
            new = jnp.maximum(old, jnp.max(scores, axis=1, keepdims=True))
            probs = jnp.exp((scores - new) * factor)
            shrink = jnp.exp((old - new) * factor)
            sum_ref[h] = sum_ref[h] * shrink + jnp.sum(probs, axis=1, keepdims=True)
            value = values[:, h * VALUE_CHANNELS:(h + 1) * VALUE_CHANNELS]
            acc_ref[h] = acc_ref[h] * shrink + dot(probs.astype(BF16), value)
            top_ref[h] = jnp.broadcast_to(new, top_ref.shape[1:])

    attend(latn_ref[...], True)

    def handle_column(slot):
        arrive(slot)
        each_column(slot, start)
        each_handled(slot, start)

    def handle_side(slot):
        arrive(slot)
        each_handled(slot, start)

    def finish(slot):
        for j in range(1, ny):
            part = lax.rem(y + j, ny) * 2 + core
            landed(slot, part)
            to_sibling(slot, part).start()
        for j in range(ny):
            landed(slot, lax.rem(y + j, ny) * 2 + 1 - core)
        attend(lat_ref[slot].reshape(length, rank + ROTARY_CHANNELS), False)

    def clean(slot, column):
        if column:
            each_column(slot, sent)
        each_handled(slot, sent)
        for j in range(1, ny):
            to_sibling(slot, lax.rem(y + j, ny) * 2 + core).wait_send()

    def side_slots(d, act):
        for j in range(1, nx):
            other = lax.rem(x + j, nx)

            @pl.when(jnp.logical_and(jnp.logical_and(d >= 0, d <= z),
                                     jnp.logical_or(d > 0, other < x)))
            def _():
                act((z - d) * nx + other)

    def round_(d, carry):
        @pl.when(d <= z)
        def _():
            handle_column((z - d) * nx + x)
        side_slots(d - 2, finish)
        side_slots(d - 1, handle_side)
        @pl.when(d <= z)
        def _():
            finish((z - d) * nx + x)
        return carry

    lax.fori_loop(1, z + 3, round_, 0)

    for h in range(att_heads):
        attended_ref[:, h * VALUE_CHANNELS:(h + 1) * VALUE_CHANNELS] = (
            acc_ref[h] / sum_ref[h]
        ).astype(BF16)

    def fold(k, carry):
        extra = states_ref[k, mem_heads * M_V:, :].astype(F32)
        state = states_ref[k, :mem_heads * M_V, :].astype(F32)
        pieces = [extra[9 * h + 3 * g:9 * h + 3 * g + 1] + extra[9 * h + 3 * g + 1:9 * h + 3 * g + 2]
                  + extra[9 * h + 3 * g + 2:9 * h + 3 * g + 3]
                  for h in range(mem_heads) for g in range(3)]
        for h in range(mem_heads):
            normal, best, last = pieces[3 * h:3 * h + 3]
            decayed = stab_ref[h:h + 1, :] + last
            new = jnp.maximum(decayed, best)
            early = jnp.exp(decayed - new)
            late = jnp.exp(best - new)
            span = slice(h * M_V, (h + 1) * M_V)
            matrix_ref[span, :] = matrix_ref[span, :] * early + late * state[span, :]
            normal_ref[h:h + 1, :] = normal_ref[h:h + 1, :] * early + late * normal
            stab_ref[h:h + 1, :] = new
        return carry

    lax.fori_loop(0, mine, fold, 0)

    squares = 0.0
    for h in range(mem_heads):
        b = stats_ref[:, 3 * h:3 * h + 1]
        local = stats_ref[:, 3 * h + 1:3 * h + 2]
        local_den = stats_ref[:, 3 * h + 2:3 * h + 3]
        q = memq_ref[:, h * M_QK:(h + 1) * M_QK]
        carried = b + stab_ref[h:h + 1, :1]
        row_max = jnp.maximum(carried, local)
        across = jnp.exp(carried - row_max)
        within = jnp.exp(local - row_max)
        inter = lax.dot_general(
            q, matrix_ref[h * M_V:(h + 1) * M_V, :].astype(BF16), NT,
            preferred_element_type=F32,
        )
        dots = jnp.sum(q.astype(F32) * normal_ref[h:h + 1, :], axis=1, keepdims=True)
        den = within * local_den + across * dots
        den = jnp.maximum(jnp.abs(den), jnp.exp(-row_max))
        cell = (within * num_ref[:, h * M_V:(h + 1) * M_V] + across * inter) / den
        cell_ref[:, h * M_V:(h + 1) * M_V] = cell
        squares = squares + jnp.sum(cell * cell, axis=1, keepdims=True)
    square_ref[...] = jnp.broadcast_to(squares, (length, 128)).T[:8]

    each_own(sent)

    def tidy(d, carry):
        @pl.when(d > 0)
        def _():
            clean((z - d) * nx + x, True)
        side_slots(d, lambda slot: clean(slot, False))
        return carry

    lax.fori_loop(0, z + 1, tidy, 0)


def project_out(tp, heads_total, cell_ref, square_ref, gate_ref, gain_ref, attended_ref,
                memory_ref, attend_ref, out_ref,
                gated_ref, squares_ref, held_ref, sib_ref, send_ref, far_ref,
                recv_q, send_q, recv_c, send_c, recv_f, send_f):
    mine = lax.axis_index("sp")
    t = lax.axis_index("tp")
    ny = tp // 2
    y = t // 2
    core = lax.rem(t, 2)
    sibling = y * 2 + 1 - core
    rows = out_ref.shape[0]
    barrier = pltpu.get_barrier_semaphore()
    for j in range(1, tp):
        pl.semaphore_signal(barrier, inc=1, device_id=(mine, lax.rem(t + j, tp)),
                            device_id_type=pl.DeviceIdType.MESH)
    pl.semaphore_wait(barrier, tp - 1)

    def remote(src, dst, send, recv, target):
        return pltpu.make_async_remote_copy(
            src_ref=src, dst_ref=dst, send_sem=send, recv_sem=recv, device_id=(mine, target),
            device_id_type=pl.DeviceIdType.MESH,
        )

    copies = [
        remote(square_ref, squares_ref.at[j - 1], send_q.at[j - 1], recv_q.at[j - 1],
               lax.rem(t + j, tp)) for j in range(1, tp)
    ]
    for copy in copies:
        copy.start()
    for copy in copies:
        copy.wait()
    total = square_ref[...]
    for j in range(tp - 1):
        total = total + squares_ref[j]
    total = jnp.concatenate([total] * 16, axis=0).T[:, :1]
    scale = lax.rsqrt(total / (heads_total * M_V) + SMALL_CONSTANT)
    opened = jax.nn.sigmoid(gate_ref[...].astype(F32))
    gated_ref[...] = (cell_ref[...] * scale * gain_ref[...].astype(F32) * opened).astype(BF16)

    def partial(owner):
        span = pl.ds(pl.multiple_of(owner * rows, rows), rows)
        return (
            dot(gated_ref[span, :], memory_ref[...]) + dot(attended_ref[span, :], attend_ref[...])
        ).astype(BF16)

    def to_sibling(j):
        return remote(held_ref.at[j], sib_ref.at[j], send_c.at[j], recv_c.at[j], sibling)

    def to_far(j):
        return remote(send_ref.at[j - 1], far_ref.at[j - 1], send_f.at[j - 1], recv_f.at[j - 1],
                      lax.rem(y + j, ny) * 2 + core)

    order = list(range(1, ny)) + [0]
    for j in order:
        chip = lax.rem(y + j, ny) * 2
        held_ref[j] = partial(chip + 1 - core)
        to_sibling(j).start()
        result = partial(chip + core).astype(F32)
        to_sibling(j).wait_recv()
        result = result + sib_ref[j].astype(F32)
        if j:
            send_ref[j - 1] = result.astype(BF16)
            to_far(j).start()
    for j in range(1, ny):
        to_far(j).wait_recv()
        result = result + far_ref[j - 1].astype(F32)
    out_ref[...] = result.astype(BF16)
    for j in order:
        to_sibling(j).wait_send()
    for j in range(1, ny):
        to_far(j).wait_send()


def params(**more):
    return pltpu.CompilerParams(vmem_limit_bytes=VMEM_LIMIT, **more)


def per_device(
    nx, tokens, input_gain, weight_query, weight_key, weight_value, weight_outgate, weight_ingate,
    weight_forget, forget_shift, mem_gain, query_down_weight, latent_down_weight, down_rotary,
    query_gain, latent_gain, query_up_weight, key_up_weight, value_up_weight, out_memory,
    out_attend,
):
    tp_index = lax.axis_index("tp")
    tp = lax.axis_size("tp")
    sp = lax.axis_size("sp")
    mem_heads = weight_query.shape[1] // M_QK
    att_heads = key_up_weight.shape[1] // PLAIN_CHANNELS
    length = tokens.shape[0] * tp
    model = tokens.shape[1]
    ingate_cols = lax.dynamic_slice_in_dim(weight_ingate, tp_index * mem_heads, mem_heads, 1)
    forget_cols = lax.dynamic_slice_in_dim(weight_forget, tp_index * mem_heads, mem_heads, 1)
    small_weight = jnp.concatenate(
        [down_rotary, ingate_cols, forget_cols,
         jnp.zeros((model, 128 - ROTARY_CHANNELS - 2 * mem_heads), BF16)], axis=1
    )
    latent_weight = jnp.concatenate([latent_down_weight, query_down_weight], axis=1)
    positions = lax.axis_index("sp") * length + jnp.arange(length, dtype=jnp.int32)
    half = ROTARY_CHANNELS // 2
    inverse = jnp.power(ROTARY_BASE, -jnp.arange(half, dtype=F32) / half)
    angles = positions.astype(F32)[:, None] * inverse
    cosine = jnp.cos(angles)
    sine = jnp.sin(angles)

    normed = rms_scale(tokens, input_gain).astype(BF16)
    rows = lax.all_gather(normed, "tp", axis=0, tiled=True)
    latents = dot(rows, latent_weight).astype(BF16)
    latents_all = lax.all_gather(latents, "tp", axis=0)
    small = dot(rows, small_weight)
    mem_query = dot(rows, weight_query).astype(BF16)
    mem_key = dot(rows, weight_key).astype(BF16)
    mem_value = dot(rows, weight_value).astype(BF16)
    mem_outgate = dot(rows, weight_outgate).astype(BF16)

    extra_rows = -(-9 * mem_heads // 32) * 32
    num, stats, state = pl.pallas_call(
        functools.partial(local_memory, mem_heads),
        out_shape=(
            jax.ShapeDtypeStruct((length, mem_heads * M_V), F32),
            jax.ShapeDtypeStruct((length, 128), F32),
            jax.ShapeDtypeStruct((mem_heads * M_V + extra_rows, 128), BF16),
        ),
        compiler_params=params(),
        name="local_memory",
    )(mem_query, mem_key, mem_value, small, forget_shift)

    query, latn = pl.pallas_call(
        functools.partial(prepare, att_heads),
        out_shape=(
            jax.ShapeDtypeStruct((att_heads, length, HEAD_WIDTH), BF16),
            jax.ShapeDtypeStruct((length, key_up_weight.shape[0] + ROTARY_CHANNELS), BF16),
        ),
        compiler_params=params(),
        name="prepare",
    )(
        latents_all, small, cosine, sine, query_gain.reshape(tp, -1), latent_gain.reshape(tp, -1),
        query_up_weight,
    )

    dma = pltpu.SemaphoreType.DMA
    cell, squares, attended = pl.pallas_call(
        functools.partial(mixers, mem_heads, att_heads, sp // nx, nx, tp),
        out_shape=(
            jax.ShapeDtypeStruct((length, mem_heads * M_V), F32),
            jax.ShapeDtypeStruct((8, length), F32),
            jax.ShapeDtypeStruct((length, att_heads * VALUE_CHANNELS), BF16),
        ),
        scratch_shapes=[
            pltpu.VMEM((sp, tp, length // tp, latn.shape[1]), BF16),
            pltpu.VMEM((sp,) + state.shape, BF16),
            pltpu.VMEM((att_heads, length, 128), F32),
            pltpu.VMEM((att_heads, length, 128), F32),
            pltpu.VMEM((att_heads, length, VALUE_CHANNELS), F32),
            pltpu.VMEM((mem_heads * M_V, 128), F32),
            pltpu.VMEM((8, 128), F32),
            pltpu.VMEM((8, 128), F32),
            dma((sp, tp)), dma((sp,)), dma((sp,)), dma((sp,)),
            dma((sp, nx)), dma((sp, nx)), dma((sp, tp // 2)), dma((sp, tp)),
        ],
        compiler_params=params(collective_id=1, has_side_effects=True),
        name="mixers",
    )(latn, state, query, key_up_weight, value_up_weight, mem_query, num, stats)

    gain_part = lax.dynamic_slice_in_dim(mem_gain, tp_index * mem_heads * M_V, mem_heads * M_V, 0)
    block = (length // tp, out_memory.shape[1])
    ny = tp // 2
    far = max(ny - 1, 1)
    return pl.pallas_call(
        functools.partial(project_out, tp, tp * mem_heads),
        out_shape=jax.ShapeDtypeStruct(block, BF16),
        scratch_shapes=[
            pltpu.VMEM((length, mem_heads * M_V), BF16),
            pltpu.VMEM((tp - 1, 8, length), F32),
            pltpu.VMEM((ny,) + block, BF16),
            pltpu.VMEM((ny,) + block, BF16),
            pltpu.VMEM((far,) + block, BF16),
            pltpu.VMEM((far,) + block, BF16),
            dma((tp - 1,)), dma((tp - 1,)), dma((ny,)), dma((ny,)), dma((far,)), dma((far,)),
        ],
        compiler_params=params(collective_id=2, has_side_effects=True),
        name="project_out",
    )(cell, squares, mem_outgate, gain_part.reshape(1, -1), attended, out_memory, out_attend)


def solution(mesh):
    placed = (
        P(("sp", "tp"), None), P(), P(None, "tp"), P(None, "tp"), P(None, "tp"), P(None, "tp"),
        P(), P(), P("sp", "tp"), P(), P(None, "tp"), P(None, "tp"), P(), P(), P(),
        P(None, "tp"), P(None, "tp"), P(None, "tp"), P("tp", None), P("tp", None),
    )
    nx = len({getattr(d, "coords", (0,))[0] for d in mesh.devices.flat})
    if mesh.shape["sp"] % nx:
        nx = 1
    return jax.shard_map(
        functools.partial(per_device, nx), mesh=mesh, in_specs=placed, out_specs=P(("sp", "tp"), None), check_vma=False
    )
```
